32 devices in a mesh: rep: 2 (over y), fs: 4 (over z), tp: 4 (over x, core).
Axes of the slice: x: 2, y: 2, z: 4, core: 2. Of those that a mesh axis runs over, the one named last changes fastest.
Arguments:
- tokens: bfloat16 [2048, 2048], P(('rep', 'fs')), may hold values from -6 to 6
- mix_gain: float32 [2048], replicated, may hold values from 0.1 to 1.9
- group_weight: float32 [512, 2048], P('fs', 'tp'), may hold values from -0.25 to 0.25
- group_scale: float32 [1, 2048], P(None, 'tp'), may hold values from 0.5 to 2
- mlp_gain: float32 [2048], replicated, may hold values from 0.1 to 1.9
- up_weight: float32 [2048, 8192], P('fs', 'tp'), may hold values from -0.125 to 0.125
- up_scale: float32 [1, 8192], P(None, 'tp'), may hold values from 0.5 to 2
- down_weight: float32 [8192, 2048], P('tp', 'fs'), may hold values from -0.0625 to 0.0625
- down_scale: float32 [1, 2048], replicated, may hold values from 0.5 to 2
Outputs:
- layer_out: bfloat16 [2048, 2048], P(('rep', 'fs'))
The draws below stay inside these ranges and needn't reach their ends.
All inputs are finite; a program needn't handle non-finite values.
Results may differ from the reference program's by a relative error of at most 0.013.
Values may be sent and summed in bfloat16 or wider, within the bound.
A program may use at most 64 MiB of HBM per device.

```python
import math
import jax
import jax.numpy as jnp
from jax import lax

D = 2048
FF = 8192
GROUPS = 4
GROUP_DIM = 512
LENGTH = 128
TOKENS = 2048
N_TP = 4


def shard_levels(stream_key, dims, cuts, smallest, high):
    level, own = 1.0, jax.random.fold_in(stream_key, 6)
    for dim, blocks in cuts:
        steps = jnp.exp(jax.random.uniform(jax.random.fold_in(own, dim), (blocks,), jnp.float32, smallest / len(cuts), high / len(cuts)))
        level = level * jnp.repeat(steps, dims[dim] // blocks).reshape([-1 if axis == dim else 1 for axis in range(len(dims))])
    return level


def gaussian(rng, shape, spread, most, shards=(), kind=jnp.bfloat16):
    values = jax.random.normal(rng, shape, jnp.float32) * spread
    if len(shards) > 0:
        values = shard_levels(rng, shape, shards, -0.22, 0.18) * values
    return jnp.clip(values, min=-most, max=most).astype(kind)


def setup_inputs(seed: int = 0) -> dict:
    keys = jax.random.split(jax.random.key(seed), 10)
    tokens = gaussian(keys[0], (TOKENS, D), 1.0, 6.0, ((0, 8),))
    mix_gain = jnp.clip(1.0 + 0.18 * jax.random.normal(keys[1], (D,), jnp.float32), 0.1, 1.9)
    group_weight = gaussian(keys[2], (GROUP_DIM, D), GROUP_DIM ** -0.5, 0.25, ((0, 4), (1, 4)), jnp.float32)
    group_scale = jnp.clip(jnp.exp(math.log(2.0) - 1.3862944 * jax.random.uniform(keys[3], (1, D), jnp.float32) ** shard_levels(keys[3], (1, D), ((1, 4),), -0.2, 0.2)), 0.5, 2.0)
    mlp_gain = jnp.clip(1.0 + 0.18 * jax.random.normal(keys[4], (D,), jnp.float32), 0.1, 1.9)
    up_weight = gaussian(keys[5], (D, FF), D ** -0.5, 0.125, ((0, 4), (1, 4)), jnp.float32)
    up_scale = jnp.clip(jnp.exp(math.log(2.0) - 1.3862944 * jax.random.uniform(keys[6], (1, FF), jnp.float32) ** shard_levels(keys[6], (1, FF), ((1, 4),), -0.2, 0.2)), 0.5, 2.0)
    down_weight = gaussian(keys[7], (FF, D), FF ** -0.5, 0.0625, ((0, 4), (1, 4)), jnp.float32)
    down_scale = jnp.clip(jnp.exp(jax.random.uniform(keys[8], (1, D), jnp.float32, math.log(0.5), math.log(2.0))), 0.5, 2.0)
    return {"tokens": tokens, "mix_gain": mix_gain, "group_weight": group_weight, "group_scale": group_scale, "mlp_gain": mlp_gain, "up_weight": up_weight, "up_scale": up_scale, "down_weight": down_weight, "down_scale": down_scale}


norm_eps = 1e-06

def norm_rows(values, gain):
    promoted = values.astype(jnp.float32)
    inverse = lax.rsqrt(lax.optimization_barrier(jnp.mean(promoted * promoted, axis=-1, keepdims=True)) + norm_eps)
    return (promoted * inverse * gain.astype(jnp.float32)).astype(jnp.bfloat16)

def band_means(inputs, window, seq_length):
    row_count, columns = inputs.shape
    by_sequence = inputs.reshape(row_count // seq_length, seq_length, columns)
    position = jnp.arange(seq_length, dtype=jnp.int32)
    offset = position[:, None] - position[None, :]
    band_mask = ((offset >= 0) & (offset < window)).astype(jnp.float32)
    divisor = jnp.minimum(position + 1, window).astype(jnp.float32)
    summed = jnp.einsum('ts,nsc->ntc', band_mask, by_sequence, precision=lax.Precision.HIGHEST)
    return (summed / divisor[None, :, None] - by_sequence).reshape(row_count, columns)

def reference(tokens, mix_gain, group_weight, group_scale, mlp_gain, up_weight, up_scale, down_weight, down_scale):
    normed = norm_rows(tokens, mix_gain).astype(jnp.float32)
    pieces = []
    for group_index in range(GROUPS):
        first_col = group_index * GROUP_DIM
        inputs = normed[:, first_col:first_col + GROUP_DIM]
        pooled = band_means(inputs, 2 ** (group_index + 1), LENGTH).astype(jnp.bfloat16)
        weight_cols = group_weight[:, first_col:first_col + GROUP_DIM].astype(jnp.bfloat16)
        product = jnp.dot(pooled, weight_cols, preferred_element_type=jnp.float32)
        pieces.append(product * group_scale[:, first_col:first_col + GROUP_DIM])
    mixed_cols = jnp.concatenate(pieces, axis=1)
    carried = (tokens.astype(jnp.float32) + mixed_cols).astype(jnp.bfloat16)
    normed_mlp = norm_rows(carried, mlp_gain)
    pre_act = jnp.dot(normed_mlp, up_weight.astype(jnp.bfloat16), preferred_element_type=jnp.float32) * up_scale
    hidden = jnp.square(jax.nn.relu(pre_act)).astype(jnp.bfloat16)
    tp_block = FF // N_TP
    summed = jnp.zeros(carried.shape, jnp.float32)
    for tp_index in range(N_TP):
        rows_here = slice(tp_index * tp_block, (tp_index + 1) * tp_block)
        partial_value = jnp.dot(hidden[:, rows_here], down_weight[rows_here].astype(jnp.bfloat16), preferred_element_type=jnp.float32) * down_scale
        summed = summed + partial_value.astype(jnp.bfloat16).astype(jnp.float32)
    return (carried.astype(jnp.float32) + summed).astype(jnp.bfloat16)
```

```python
import functools

import jax
import jax.numpy as jnp
from jax import lax
from jax.experimental import pallas as pl
from jax.experimental.pallas import tpu as pltpu
from jax.sharding import PartitionSpec as P

GROUPS = 4
LENGTH = 128


norm_eps = 1e-06


def norm_rows(values, gain):
    promoted = values.astype(jnp.float32)
    inverse = lax.rsqrt(jnp.mean(promoted * promoted, axis=-1, keepdims=True) + norm_eps)
    return (promoted * inverse * gain).astype(jnp.bfloat16)


def band_means(inputs, window, seq_length):
    row_count, columns = inputs.shape
    by_sequence = inputs.reshape(row_count // seq_length, seq_length, columns)
    position = jnp.arange(seq_length, dtype=jnp.int32)
    offset = position[:, None] - position[None, :]
    band_mask = ((offset >= 0) & (offset < window)).astype(jnp.bfloat16)
    divisor = jnp.minimum(position + 1, window).astype(jnp.float32)
    summed = jnp.einsum("ts,nsc->ntc", band_mask, by_sequence, preferred_element_type=jnp.float32)
    return (summed / divisor[None, :, None] - by_sequence.astype(jnp.float32)).reshape(
        row_count, columns
    )


def body(
    tokens,
    mix_gain,
    group_weight,
    group_scale,
    mlp_gain,
    up_weight,
    up_scale,
    down_weight,
    down_scale,
):
    model_width = tokens.shape[1]
    group_width = model_width // GROUPS
    own_cols = group_weight.shape[1]
    column_start = lax.axis_index("tp") * own_cols
    group_index = column_start // group_width
    normed = norm_rows(tokens, mix_gain)
    inputs = lax.dynamic_slice_in_dim(normed, group_index * group_width, group_width, 1)
    window = jnp.left_shift(jnp.int32(2), group_index)
    pooled = band_means(inputs, window, LENGTH).astype(jnp.bfloat16)
    mixed_cols = (
        jnp.dot(
            pooled,
            lax.all_gather(group_weight.astype(jnp.bfloat16), "fs", axis=0, tiled=True),
            preferred_element_type=jnp.float32,
        )
        * group_scale
    )
    own_tokens = lax.dynamic_slice_in_dim(tokens, column_start, own_cols, 1)
    carried_cols = (own_tokens.astype(jnp.float32) + mixed_cols).astype(jnp.bfloat16)
    carried = lax.all_gather(carried_cols, "tp", axis=1, tiled=True)
    normed_mlp = norm_rows(carried, mlp_gain)
    pre_act = (
        jnp.dot(
            normed_mlp,
            lax.all_gather(up_weight.astype(jnp.bfloat16), "fs", axis=0, tiled=True),
            preferred_element_type=jnp.float32,
        )
        * up_scale
    )
    hidden = jnp.square(jax.nn.relu(pre_act)).astype(jnp.bfloat16)
    partial_value = (
        jnp.dot(
            hidden,
            lax.all_gather(down_weight.astype(jnp.bfloat16), "fs", axis=1, tiled=True),
            preferred_element_type=jnp.float32,
        )
        * down_scale
    )
    summed = lax.psum(partial_value.astype(jnp.bfloat16), "tp").astype(jnp.float32)
    return (carried.astype(jnp.float32) + summed).astype(jnp.bfloat16)


MESH = pl.DeviceIdType.MESH


def ring_kernel(
    sizes,
    tok_h, mg, gw_h, gs, lg, up_h, us, dn_h, ds,
    out_h,
    tok, gwf, upf, upo, dnf, dno,
    gwg, ups, upg, dns, dng,
    car, xn, pb, ra, sx, rb, sz, rc, og,
    ld, sw, rw, sy, ry, scz, rcz, scx, rcx, scc, rcc,
    sa, ra_s, sb, rb_s, st, rt, so, ro, wr,
):
    Z, T, rows, D, own, hg, hu, hd, fsub, dsub = sizes
    r, z, t = lax.axis_index("rep"), lax.axis_index("fs"), lax.axis_index("tp")
    cp = t + 1 - 2 * lax.rem(t, 2)
    xp = lax.rem(t + 2, T)
    cxp = lax.rem(cp + 2, T)
    peer_r = 1 - r
    bf, f32 = jnp.bfloat16, jnp.float32

    def mul(i, n):
        return pl.multiple_of(i * n, n)

    def zat(d):
        return lax.rem(z + d, Z)

    loads = {}

    def load(key, src, dst, k):
        c = pltpu.make_async_copy(src, dst, ld.at[k])
        c.start()
        loads[key] = c

    load("gw", gw_h, gwf, 0)
    load("tok", tok_h, tok, 1)
    order = list(range(1, Z)) + [0]
    for i, d in enumerate(order):
        zd = zat(d)
        load(("up", d), up_h.at[pl.ds(mul(r, hu), hu), pl.ds(mul(zd, fsub), fsub)], upf.at[d], 2 + d)
        load(("dn", d), dn_h.at[pl.ds(pl.multiple_of(zd * 2 * hd + r * hd, hd), hd), :], dnf.at[d], 2 + Z + d)
    load("upo", up_h.at[pl.ds(mul(peer_r, hu), hu), pl.ds(mul(z, fsub), fsub)], upo, 2 + 2 * Z)
    load("dno", dn_h.at[pl.ds(pl.multiple_of(z * 2 * hd + peer_r * hd, hd), hd), :], dno, 3 + 2 * Z)

    barrier = pltpu.get_barrier_semaphore()
    peers = [(r, zat(d), t) for d in range(1, Z)] + [(peer_r, z, t), (r, z, xp), (r, z, cp)]
    for p in peers:
        pl.semaphore_signal(barrier, inc=1, device_id=p, device_id_type=MESH)
    pl.semaphore_wait(barrier, len(peers))

    sends = []

    def remote(src, dst, ss, rs, dev):
        return pltpu.make_async_remote_copy(
            src_ref=src, dst_ref=dst, send_sem=ss, recv_sem=rs, device_id=dev, device_id_type=MESH
        )

    def send(src, dst, ss, rs, dev):
        c = remote(src, dst, ss, rs, dev)
        c.start()
        sends.append(c)

    def got(dst, ss, rs):
        remote(dst, dst, ss, rs, (peer_r, z, t)).wait_recv()

    def gw_at(src, rep):
        return gwg.at[pl.ds(pl.multiple_of(src * 2 * hg + rep * hg, hg), hg), :]

    def up_at(src, rep):
        return upg.at[pl.ds(pl.multiple_of(src * 2 * hu + rep * hu, hu), hu), :]

    def dn_at(src, rep):
        return dng.at[src, pl.ds(mul(rep, hd), hd), :]

    place = (gw_at, up_at, dn_at)

    loads["gw"].wait()
    gwg[pl.ds(mul(z, 2 * hg), 2 * hg), :] = gwf[...].astype(bf)
    for i, d in enumerate(range(1, Z)):
        loads[("up", d)].wait()
        ups[d] = upf[d].astype(bf)
        if i == 0:
            for e in range(1, Z):
                send(gw_at(z, r), gw_at(z, r), sw.at[0, e], rw.at[0, z], (r, zat(e), t))
        loads[("dn", d)].wait()
        dns[d] = dnf[d].astype(bf)
    for d in range(1, Z):
        send(ups.at[d], up_at(z, r), sw.at[1, d], rw.at[1, z], (r, zat(d), t))
    for d in range(1, Z):
        send(dns.at[d], dn_at(z, r), sw.at[2, d], rw.at[2, z], (r, zat(d), t))
    loads[("up", 0)].wait()
    upg[pl.ds(pl.multiple_of(z * 2 * hu + r * hu, hu), hu), :] = upf[0].astype(bf)
    loads["upo"].wait()
    upg[pl.ds(pl.multiple_of(z * 2 * hu + peer_r * hu, hu), hu), :] = upo[...].astype(bf)
    loads[("dn", 0)].wait()
    dng[z, pl.ds(mul(r, hd), hd), :] = dnf[0].astype(bf)
    loads["dno"].wait()
    dng[z, pl.ds(mul(peer_r, hd), hd), :] = dno[...].astype(bf)

    loads["tok"].wait()
    full = tok[...].astype(f32)
    inv = lax.rsqrt(jnp.mean(full * full, axis=-1, keepdims=True) + norm_eps)
    cols = pl.ds(mul(t, own), own)
    mine = tok[:, cols].astype(f32)
    normed = (mine * inv * mg[:, cols]).astype(bf)
    window = jnp.left_shift(jnp.int32(2), t)
    ti = lax.broadcasted_iota(jnp.int32, (LENGTH, LENGTH), 0)
    si = lax.broadcasted_iota(jnp.int32, (LENGTH, LENGTH), 1)
    band = jnp.where((ti - si >= 0) & (ti - si < window), 1.0, 0.0).astype(bf)
    pos = lax.broadcasted_iota(jnp.int32, (LENGTH, own), 0)
    divisor = jnp.minimum(pos + 1, window).astype(f32)
    pooled = []
    for s in range(rows // LENGTH):
        part = normed[s * LENGTH:(s + 1) * LENGTH]
        summed = jnp.dot(band, part, preferred_element_type=f32)
        pooled.append((summed / divisor - part.astype(f32)).astype(bf))
    pooled = jnp.concatenate(pooled, axis=0)

    def swap(w):
        for d in range(1, Z):
            src = zat(Z - d)
            got(place[w](src, r), sw.at[w, d], rw.at[w, src])
            send(place[w](src, r), place[w](src, r), sy.at[w, d], ry.at[w, src], (peer_r, z, t))

    def swapped(w):
        for d in range(1, Z):
            src = zat(Z - d)
            got(place[w](src, peer_r), sy.at[w, d], ry.at[w, src])

    swap(0)
    swapped(0)
    mixed = jnp.dot(pooled, gwg[...], preferred_element_type=f32) * gs[...]
    car[z, t] = (mine + mixed).astype(bf)
    blk = car.at[z, t]
    send(blk, blk, scx.at[0], rcx.at[z], (r, z, xp))
    send(blk, blk, scc.at[0, 0], rcc.at[z, 0], (r, z, cp))
    for d in range(1, Z):
        send(blk, blk, scz.at[d], rcz.at[z], (r, zat(d), t))

    def from_x(d):
        src = zat(Z - d)
        got(car.at[src, xp], scx.at[d], rcx.at[src])
        b = car.at[src, xp]
        send(b, b, scc.at[d, 1], rcc.at[src, 1], (r, z, cp))

    swap(1)
    from_x(0)
    swap(2)
    for d in range(1, Z):
        src = zat(Z - d)
        b = car.at[src, t]
        got(b, scz.at[d], rcz.at[src])
        send(b, b, scx.at[d], rcx.at[src], (r, z, xp))
        send(b, b, scc.at[d, 0], rcc.at[src, 0], (r, z, cp))
    swapped(1)
    swapped(2)

    def compute(d):
        src = zat(Z - d)
        if d > 0:
            from_x(d)
        got(car.at[src, cp], scc.at[d, 0], rcc.at[src, 0])
        got(car.at[src, cxp], scc.at[d, 1], rcc.at[src, 1])
        total = jnp.zeros((rows, 1), f32)
        for q in range(T):
            c = car[src, q].astype(f32)
            total += jnp.sum(c * c, axis=-1, keepdims=True)
        scale = lax.rsqrt(total / D + norm_eps)
        for q in range(T):
            part = slice(q * own, (q + 1) * own)
            xn[:, part] = (car[src, q].astype(f32) * scale * lg[:, part]).astype(bf)
        pre = jnp.dot(xn[...], upg[...], preferred_element_type=f32)
        pre = jnp.maximum(pre * us[:, pl.ds(mul(z, fsub), fsub)], 0.0)
        hidden = (pre * pre).astype(bf)
        for q in range(T):
            part = slice(q * own, (q + 1) * own)
            p = jnp.dot(hidden, dng[q], preferred_element_type=f32) * ds[:, part]
            pb[src, q] = p.astype(bf)
        send(pb.at[src, cxp], ra.at[src, 1], sa.at[d, 1], ra_s.at[src, 1], (r, z, cp))
        send(pb.at[src, cp], ra.at[src, 0], sa.at[d, 0], ra_s.at[src, 0], (r, z, cp))

    def over_x(d):
        src = zat(Z - d)
        got(ra.at[src, 1], sa.at[d, 1], ra_s.at[src, 1])
        sx[src] = (pb[src, xp].astype(f32) + ra[src, 1].astype(f32)).astype(bf)
        send(sx.at[src], rb.at[src], sb.at[d], rb_s.at[src], (r, z, xp))

    def over_z(d):
        src = zat(Z - d)
        got(ra.at[src, 0], sa.at[d, 0], ra_s.at[src, 0])
        got(rb.at[src], sb.at[d], rb_s.at[src])
        both = pb[src, t].astype(f32) + ra[src, 0].astype(f32) + rb[src].astype(f32)
        if d == 0:
            return both
        sz[src] = both.astype(bf)
        send(sz.at[src], rc.at[z], st.at[d], rt.at[z], (r, src, t))

    kept = None
    for i in range(Z + 2):
        if i < Z:
            compute(i)
        if 0 <= i - 1 < Z:
            over_x(i - 1)
        if 0 <= i - 2 < Z:
            if i - 2 > 0:
                over_z(i - 2)
    acc = over_z(0)
    acc += car[z, t].astype(f32)
    for d in range(1, Z):
        src = zat(d)
        got(rc.at[src], st.at[d], rt.at[src])
        acc += rc[src].astype(f32)
    og[t] = acc.astype(bf)
    send(og.at[t], og.at[t], so.at[0], ro.at[0], (r, z, xp))
    send(og.at[t], og.at[t], so.at[1], ro.at[1], (r, z, cp))
    writes = []

    def write(q, k):
        c = pltpu.make_async_copy(og.at[q], out_h.at[:, pl.ds(mul(q, own), own)], wr.at[k])
        c.start()
        writes.append(c)

    write(t, 0)
    got(og.at[xp], so.at[0], ro.at[0])
    send(og.at[xp], og.at[xp], so.at[2], ro.at[2], (r, z, cp))
    write(xp, 1)
    got(og.at[cp], so.at[1], ro.at[1])
    write(cp, 2)
    got(og.at[cxp], so.at[2], ro.at[2])
    write(cxp, 3)
    for c in sends:
        c.wait_send()
    for c in writes:
        c.wait()


def fused(mesh_shape, tokens, mix_gain, group_weight, group_scale, mlp_gain, up_weight, up_scale, down_weight, down_scale):
    Z, T = mesh_shape["fs"], mesh_shape["tp"]
    rows, D = tokens.shape
    own = group_weight.shape[1]
    hg, hu = group_weight.shape[0] // 2, up_weight.shape[0] // 2
    fsub = up_weight.shape[1] // Z
    hd = fsub // 2
    dsub = down_weight.shape[1]
    bf, f32 = jnp.bfloat16, jnp.float32
    dma = pltpu.SemaphoreType.DMA
    vm = pl.BlockSpec(memory_space=pltpu.VMEM)
    hbm = pl.BlockSpec(memory_space=pl.ANY)
    sizes = (Z, T, rows, D, own, hg, hu, hd, fsub, dsub)
    V = pltpu.VMEM
    block = (Z, rows, own)
    return pl.pallas_call(
        functools.partial(ring_kernel, sizes),
        out_shape=jax.ShapeDtypeStruct((rows, D), bf),
        in_specs=[hbm, vm, hbm, vm, vm, hbm, vm, hbm, vm],
        out_specs=hbm,
        scratch_shapes=[
            V((rows, D), bf), V((2 * hg, own), f32),
            V((Z, hu, fsub), f32), V((hu, fsub), f32), V((Z, hd, dsub), f32), V((hd, dsub), f32),
            V((Z * 2 * hg, own), bf), V((Z, hu, fsub), bf), V((Z * 2 * hu, fsub), bf),
            V((Z, hd, dsub), bf), V((Z, 2 * hd, dsub), bf),
            V((Z, T, rows, own), bf), V((rows, D), bf), V((Z, T, rows, own), bf),
            V((Z, 2, rows, own), bf), V(block, bf), V(block, bf), V(block, bf), V(block, bf),
            V((T, rows, own), bf),
            dma((4 + 2 * Z,)), dma((3, Z)), dma((3, Z)), dma((3, Z)), dma((3, Z)),
            dma((Z,)), dma((Z,)), dma((Z,)), dma((Z,)), dma((Z, 2)), dma((Z, 2)),
            dma((Z, 2)), dma((Z, 2)), dma((Z,)), dma((Z,)), dma((Z,)), dma((Z,)),
            dma((3,)), dma((3,)), dma((4,)),
        ],
        compiler_params=pltpu.CompilerParams(
            collective_id=0, has_side_effects=True, vmem_limit_bytes=60 * 1024 * 1024
        ),
    )(
        tokens, mix_gain[None], group_weight, group_scale, mlp_gain[None],
        up_weight, up_scale, down_weight, down_scale,
    )


def fits(mesh):
    shape = mesh.shape
    return shape["rep"] == 2 and shape["tp"] == GROUPS and shape["fs"] == shape["tp"]


def solution(mesh):
    in_specs = (
        P(("rep", "fs"), None),
        P(),
        P("fs", "tp"),
        P(None, "tp"),
        P(),
        P("fs", "tp"),
        P(None, "tp"),
        P("tp", "fs"),
        P(),
    )
    out_specs = P(("rep", "fs"), None)
    chosen = functools.partial(fused, mesh.shape) if fits(mesh) else body
    return jax.shard_map(chosen, mesh=mesh, in_specs=in_specs, out_specs=out_specs, check_vma=False)
```

```python
import functools

import jax
import jax.numpy as jnp
from jax import lax
from jax.experimental import pallas as pl
from jax.experimental.pallas import tpu as pltpu
from jax.sharding import PartitionSpec as P

GROUPS = 4
LENGTH = 128


norm_eps = 1e-06


def norm_rows(values, gain):
    promoted = values.astype(jnp.float32)
    inverse = lax.rsqrt(jnp.mean(promoted * promoted, axis=-1, keepdims=True) + norm_eps)
    return (promoted * inverse * gain).astype(jnp.bfloat16)


def band_means(inputs, window, seq_length):
    row_count, columns = inputs.shape
    by_sequence = inputs.reshape(row_count // seq_length, seq_length, columns)
    position = jnp.arange(seq_length, dtype=jnp.int32)
    offset = position[:, None] - position[None, :]
    band_mask = ((offset >= 0) & (offset < window)).astype(jnp.bfloat16)
    divisor = jnp.minimum(position + 1, window).astype(jnp.float32)
    summed = jnp.einsum("ts,nsc->ntc", band_mask, by_sequence, preferred_element_type=jnp.float32)
    return (summed / divisor[None, :, None] - by_sequence.astype(jnp.float32)).reshape(
        row_count, columns
    )


def body(
    tokens,
    mix_gain,
    group_weight,
    group_scale,
    mlp_gain,
    up_weight,
    up_scale,
    down_weight,
    down_scale,
):
    model_width = tokens.shape[1]
    group_width = model_width // GROUPS
    own_cols = group_weight.shape[1]
    column_start = lax.axis_index("tp") * own_cols
    group_index = column_start // group_width
    normed = norm_rows(tokens, mix_gain)
    inputs = lax.dynamic_slice_in_dim(normed, group_index * group_width, group_width, 1)
    window = jnp.left_shift(jnp.int32(2), group_index)
    pooled = band_means(inputs, window, LENGTH).astype(jnp.bfloat16)
    mixed_cols = (
        jnp.dot(
            pooled,
            lax.all_gather(group_weight.astype(jnp.bfloat16), "fs", axis=0, tiled=True),
            preferred_element_type=jnp.float32,
        )
        * group_scale
    )
    own_tokens = lax.dynamic_slice_in_dim(tokens, column_start, own_cols, 1)
    carried_cols = (own_tokens.astype(jnp.float32) + mixed_cols).astype(jnp.bfloat16)
    carried = lax.all_gather(carried_cols, "tp", axis=1, tiled=True)
    normed_mlp = norm_rows(carried, mlp_gain)
    pre_act = (
        jnp.dot(
            normed_mlp,
            lax.all_gather(up_weight.astype(jnp.bfloat16), "fs", axis=0, tiled=True),
            preferred_element_type=jnp.float32,
        )
        * up_scale
    )
    hidden = jnp.square(jax.nn.relu(pre_act)).astype(jnp.bfloat16)
    partial_value = (
        jnp.dot(
            hidden,
            lax.all_gather(down_weight.astype(jnp.bfloat16), "fs", axis=1, tiled=True),
            preferred_element_type=jnp.float32,
        )
        * down_scale
    )
    summed = lax.psum(partial_value.astype(jnp.bfloat16), "tp").astype(jnp.float32)
    return (carried.astype(jnp.float32) + summed).astype(jnp.bfloat16)


MESH = pl.DeviceIdType.MESH


def ring_kernel(
    sizes,
    tok_h, mg, gw_h, gs, lg, up_h, us, dn_h, ds,
    out_h,
    tok, gwf, upf, upo, dnf, dno,
    gwg, ups, upg, dns, dng,
    car, xn, pb, ra, sx, rb, sz, rc, og,
    ld, sw, rw, sy, ry, scz, rcz, scx, rcx, scc, rcc,
    sa, ra_s, sb, rb_s, st, rt, so, ro, wr,
):
    Z, T, rows, D, own, hg, hu, hd, fsub, dsub = sizes
    r, z, t = lax.axis_index("rep"), lax.axis_index("fs"), lax.axis_index("tp")
    cp = t + 1 - 2 * lax.rem(t, 2)
    xp = lax.rem(t + 2, T)
    cxp = lax.rem(cp + 2, T)
    peer_r = 1 - r
    bf, f32 = jnp.bfloat16, jnp.float32

    def mul(i, n):
        return pl.multiple_of(i * n, n)

    def zat(d):
        return lax.rem(z + d, Z)

    loads = {}

    def load(key, src, dst, k):
        c = pltpu.make_async_copy(src, dst, ld.at[k])
        c.start()
        loads[key] = c

    load("gw", gw_h, gwf, 0)
    load("tok", tok_h, tok, 1)
    order = list(range(1, Z)) + [0]
    for d in order:
        zd = zat(d)
        load(("up", d), up_h.at[pl.ds(mul(r, hu), hu), pl.ds(mul(zd, fsub), fsub)], upf.at[d], 2 + d)
    for d in order:
        zd = zat(d)
        load(("dn", d), dn_h.at[pl.ds(pl.multiple_of(zd * 2 * hd + r * hd, hd), hd), :], dnf.at[d], 2 + Z + d)
    load("upo", up_h.at[pl.ds(mul(peer_r, hu), hu), pl.ds(mul(z, fsub), fsub)], upo, 2 + 2 * Z)
    load("dno", dn_h.at[pl.ds(pl.multiple_of(z * 2 * hd + peer_r * hd, hd), hd), :], dno, 3 + 2 * Z)

    barrier = pltpu.get_barrier_semaphore()
    peers = [(r, zat(d), t) for d in range(1, Z)] + [(peer_r, z, t), (r, z, xp), (r, z, cp)]
    for p in peers:
        pl.semaphore_signal(barrier, inc=1, device_id=p, device_id_type=MESH)
    loads["gw"].wait()
    gwg[pl.ds(mul(z, 2 * hg), 2 * hg), :] = gwf[...].astype(bf)
    pl.semaphore_wait(barrier, len(peers))

    sends = []

    def remote(src, dst, ss, rs, dev):
        return pltpu.make_async_remote_copy(
            src_ref=src, dst_ref=dst, send_sem=ss, recv_sem=rs, device_id=dev, device_id_type=MESH
        )

    def send(src, dst, ss, rs, dev, when=None):
        if when is None:
            remote(src, dst, ss, rs, dev).start()
        else:
            pl.when(when)(lambda: remote(src, dst, ss, rs, dev).start())
        sends.append((when, (src, dst, ss, rs, dev)))

    def drain():
        for when, args in sends:
            if when is None:
                remote(*args).wait_send()
            else:
                pl.when(when)(lambda args=args: remote(*args).wait_send())

    def got(dst, ss, rs):
        remote(dst, dst, ss, rs, (peer_r, z, t)).wait_recv()

    def gw_at(src, rep):
        return gwg.at[pl.ds(pl.multiple_of(src * 2 * hg + rep * hg, hg), hg), :]

    def up_at(src, rep):
        return upg.at[pl.ds(pl.multiple_of(src * 2 * hu + rep * hu, hu), hu), :]

    def dn_at(src, rep):
        return dng.at[src, pl.ds(mul(rep, hd), hd), :]

    place = (gw_at, up_at, dn_at)

    for d in range(1, Z):
        send(gw_at(z, r), gw_at(z, r), sw.at[0, d], rw.at[0, z], (r, zat(d), t))
    ready = []
    for w, key, raw, cast in ((1, "up", upf, ups), (2, "dn", dnf, dns)):
        for d in range(1, Z):
            loads[(key, d)].wait()
            cast[d] = raw[d].astype(bf)
            ready.append((cast.at[d], place[w](z, r), sw.at[w, d], rw.at[w, z], (r, zat(d), t)))
            if len(ready) > 1:
                send(*ready.pop(0))
    send(*ready.pop(0))
    loads[("up", 0)].wait()
    upg[pl.ds(pl.multiple_of(z * 2 * hu + r * hu, hu), hu), :] = upf[0].astype(bf)
    loads["upo"].wait()
    upg[pl.ds(pl.multiple_of(z * 2 * hu + peer_r * hu, hu), hu), :] = upo[...].astype(bf)
    loads[("dn", 0)].wait()
    dng[z, pl.ds(mul(r, hd), hd), :] = dnf[0].astype(bf)
    loads["dno"].wait()
    dng[z, pl.ds(mul(peer_r, hd), hd), :] = dno[...].astype(bf)

    loads["tok"].wait()
    full = tok[...].astype(f32)
    inv = lax.rsqrt(jnp.mean(full * full, axis=-1, keepdims=True) + norm_eps)
    cols = pl.ds(mul(t, own), own)
    mine = tok[:, cols].astype(f32)
    normed = (mine * inv * mg[:, cols]).astype(bf)
    window = jnp.left_shift(jnp.int32(2), t)
    ti = lax.broadcasted_iota(jnp.int32, (LENGTH, LENGTH), 0)
    si = lax.broadcasted_iota(jnp.int32, (LENGTH, LENGTH), 1)
    band = jnp.where((ti - si >= 0) & (ti - si < window), 1.0, 0.0).astype(bf)
    pos = lax.broadcasted_iota(jnp.int32, (LENGTH, own), 0)
    divisor = jnp.minimum(pos + 1, window).astype(f32)
    pooled = []
    for s in range(rows // LENGTH):
        part = normed[s * LENGTH:(s + 1) * LENGTH]
        summed = jnp.dot(band, part, preferred_element_type=f32)
        pooled.append((summed / divisor - part.astype(f32)).astype(bf))
    pooled = jnp.concatenate(pooled, axis=0)

    def swap(w):
        for d in range(1, Z):
            src = zat(Z - d)
            got(place[w](src, r), sw.at[w, d], rw.at[w, src])
            send(place[w](src, r), place[w](src, r), sy.at[w, d], ry.at[w, src], (peer_r, z, t))

    def swapped(w):
        for d in range(1, Z):
            src = zat(Z - d)
            got(place[w](src, peer_r), sy.at[w, d], ry.at[w, src])

    swap(0)
    swapped(0)
    mixed = jnp.dot(pooled, gwg[...], preferred_element_type=f32) * gs[...]
    car[z, t] = (mine + mixed).astype(bf)
    H = rows // LENGTH
    hr = LENGTH
    side = 1 - 2 * lax.div(z, Z // 2)

    inner = lax.div(Z - 1 - side * (Z - 1 - 2 * z), 2)

    def src_of(d):
        if d == 0:
            return z
        near = (d + 1) // 2 if d % 2 else -(d // 2)
        both_sides = lax.div(2 * inner - d + 2 * Z, 2 * Z)
        return z + side * (both_sides * near + (1 - both_sides) * (d - inner))

    def half(h):
        return pl.ds(h * hr, hr)

    def to_x(src, h):
        b = car.at[src, t, half(h)]
        send(b, b, scx.at[src, h], rcx.at[src, h], (r, z, xp))

    def to_core(src, h, q, k):
        b = car.at[src, q, half(h)]
        send(b, b, scc.at[src, k, h], rcc.at[src, k, h], (r, z, cp))

    def to_z(src, h, when_up, when_down):
        b = car.at[src, t, half(h)]
        send(b, b, scz.at[0, src, h], rcz.at[src, h], (r, lax.rem(z + 1, Z), t), when_up)
        send(b, b, scz.at[1, src, h], rcz.at[src, h], (r, lax.rem(z + Z - 1, Z), t), when_down)

    for h in range(H):
        to_z(z, h, z < Z - 1, z > 0)
        to_x(z, h)
        to_core(z, h, t, 0)

    def arrive(d, h):
        src = src_of(d)
        got(car.at[src, t, half(h)], scz.at[0, src, h], rcz.at[src, h])
        to_z(src, h, (src < z) & (z < Z - 1), (src > z) & (z > 0))
        to_x(src, h)
        to_core(src, h, t, 0)

    def from_x(d, h):
        src = src_of(d)
        got(car.at[src, xp, half(h)], scx.at[src, h], rcx.at[src, h])
        to_core(src, h, xp, 1)

    swap(1)
    for h in range(H):
        from_x(0, h)
    swap(2)
    swapped(1)
    swapped(2)

    def compute(d, h):
        src = src_of(d)
        hs = half(h)
        got(car.at[src, cp, hs], scc.at[src, 0, h], rcc.at[src, 0, h])
        got(car.at[src, cxp, hs], scc.at[src, 1, h], rcc.at[src, 1, h])
        total = jnp.zeros((hr, 1), f32)
        for q in range(T):
            c = car[src, q, hs].astype(f32)
            total += jnp.sum(c * c, axis=-1, keepdims=True)
        scale = lax.rsqrt(total / D + norm_eps)
        for q in range(T):
            part = slice(q * own, (q + 1) * own)
            xn[:, part] = (car[src, q, hs].astype(f32) * scale * lg[:, part]).astype(bf)
        pre = jnp.dot(xn[...], upg[...], preferred_element_type=f32)
        pre = jnp.maximum(pre * us[:, pl.ds(mul(z, fsub), fsub)], 0.0)
        hidden = (pre * pre).astype(bf)
        for q in range(T):
            part = slice(q * own, (q + 1) * own)
            p = jnp.dot(hidden, dng[q], preferred_element_type=f32) * ds[:, part]
            pb[src, q, hs] = p.astype(bf)
        for k, q in ((1, cxp), (0, cp)):
            send(pb.at[src, q, hs], ra.at[src, k, hs], sa.at[src, k, h], ra_s.at[src, k, h], (r, z, cp))

    def over_x(d, h):
        src = src_of(d)
        hs = half(h)
        got(ra.at[src, 1, hs], sa.at[src, 1, h], ra_s.at[src, 1, h])
        sx[src, hs] = (pb[src, xp, hs].astype(f32) + ra[src, 1, hs].astype(f32)).astype(bf)
        send(sx.at[src, hs], rb.at[src, hs], sb.at[src, h], rb_s.at[src, h], (r, z, xp))

    def over_z(d, h):
        src = src_of(d)
        hs = half(h)
        got(ra.at[src, 0, hs], sa.at[src, 0, h], ra_s.at[src, 0, h])
        got(rb.at[src, hs], sb.at[src, h], rb_s.at[src, h])
        both = pb[src, t, hs].astype(f32) + ra[src, 0, hs].astype(f32) + rb[src, hs].astype(f32)
        if d == 0:
            return both
        sz[src, hs] = both.astype(bf)
        send(sz.at[src, hs], rc.at[z, hs], st.at[src, h], rt.at[z, h], (r, src, t))

    units = [(d, h) for d in range(Z) for h in range(H)]
    lead = 4
    for i in range(len(units) + lead):
        for lag, stage in enumerate((arrive, from_x, compute, over_x, over_z)):
            if 0 <= i - lag < len(units):
                d, h = units[i - lag]
                if d > 0 or stage in (compute, over_x):
                    stage(d, h)

    writes = []

    def write(q, k, h):
        c = pltpu.make_async_copy(
            og.at[q, half(h)], out_h.at[half(h), pl.ds(mul(q, own), own)], wr.at[k, h]
        )
        c.start()
        writes.append(c)

    def pass_on(q, k, dev, h):
        b = og.at[q, half(h)]
        send(b, b, so.at[k, h], ro.at[k, h], dev)

    for h in range(H):
        hs = half(h)
        acc = over_z(0, h) + car[z, t, hs].astype(f32)
        for d in range(1, Z):
            src = src_of(d)
            got(rc.at[src, hs], st.at[src, h], rt.at[src, h])
            acc += rc[src, hs].astype(f32)
        og[t, hs] = acc.astype(bf)
        pass_on(t, 0, (r, z, xp), h)
        pass_on(t, 1, (r, z, cp), h)
        write(t, 0, h)
    for h in range(H):
        got(og.at[xp, half(h)], so.at[0, h], ro.at[0, h])
        pass_on(xp, 2, (r, z, cp), h)
        write(xp, 1, h)
    for h in range(H):
        got(og.at[cp, half(h)], so.at[1, h], ro.at[1, h])
        write(cp, 2, h)
        got(og.at[cxp, half(h)], so.at[2, h], ro.at[2, h])
        write(cxp, 3, h)
    drain()
    for c in writes:
        c.wait()


def fused(mesh_shape, tokens, mix_gain, group_weight, group_scale, mlp_gain, up_weight, up_scale, down_weight, down_scale):
    Z, T = mesh_shape["fs"], mesh_shape["tp"]
    rows, D = tokens.shape
    own = group_weight.shape[1]
    hg, hu = group_weight.shape[0] // 2, up_weight.shape[0] // 2
    fsub = up_weight.shape[1] // Z
    hd = fsub // 2
    dsub = down_weight.shape[1]
    bf, f32 = jnp.bfloat16, jnp.float32
    dma = pltpu.SemaphoreType.DMA
    vm = pl.BlockSpec(memory_space=pltpu.VMEM)
    hbm = pl.BlockSpec(memory_space=pl.ANY)
    sizes = (Z, T, rows, D, own, hg, hu, hd, fsub, dsub)
    V = pltpu.VMEM
    block = (Z, rows, own)
    H = rows // LENGTH
    return pl.pallas_call(
        functools.partial(ring_kernel, sizes),
        out_shape=jax.ShapeDtypeStruct((rows, D), bf),
        in_specs=[hbm, vm, hbm, vm, vm, hbm, vm, hbm, vm],
        out_specs=hbm,
        scratch_shapes=[
            V((rows, D), bf), V((2 * hg, own), f32),
            V((Z, hu, fsub), f32), V((hu, fsub), f32), V((Z, hd, dsub), f32), V((hd, dsub), f32),
            V((Z * 2 * hg, own), bf), V((Z, hu, fsub), bf), V((Z * 2 * hu, fsub), bf),
            V((Z, hd, dsub), bf), V((Z, 2 * hd, dsub), bf),
            V((Z, T, rows, own), bf), V((LENGTH, D), bf), V((Z, T, rows, own), bf),
            V((Z, 2, rows, own), bf), V(block, bf), V(block, bf), V(block, bf), V(block, bf),
            V((T, rows, own), bf),
            dma((4 + 2 * Z,)), dma((3, Z)), dma((3, Z)), dma((3, Z)), dma((3, Z)),
            dma((2, Z, H)), dma((Z, H)), dma((Z, H)), dma((Z, H)), dma((Z, 2, H)), dma((Z, 2, H)),
            dma((Z, 2, H)), dma((Z, 2, H)), dma((Z, H)), dma((Z, H)), dma((Z, H)), dma((Z, H)),
            dma((3, H)), dma((3, H)), dma((4, H)),
        ],
        compiler_params=pltpu.CompilerParams(
            collective_id=0, has_side_effects=True, vmem_limit_bytes=60 * 1024 * 1024
        ),
    )(
        tokens, mix_gain[None], group_weight, group_scale, mlp_gain[None],
        up_weight, up_scale, down_weight, down_scale,
    )


def fits(mesh):
    shape = mesh.shape
    return shape["rep"] == 2 and shape["tp"] == GROUPS and shape["fs"] == shape["tp"]


def solution(mesh):
    in_specs = (
        P(("rep", "fs"), None),
        P(),
        P("fs", "tp"),
        P(None, "tp"),
        P(),
        P("fs", "tp"),
        P(None, "tp"),
        P("tp", "fs"),
        P(),
    )
    out_specs = P(("rep", "fs"), None)
    chosen = functools.partial(fused, mesh.shape) if fits(mesh) else body
    return jax.shard_map(chosen, mesh=mesh, in_specs=in_specs, out_specs=out_specs, check_vma=False)
```

```python
import functools

import jax
import jax.numpy as jnp
from jax import lax
from jax.experimental import pallas as pl
from jax.experimental.pallas import tpu as pltpu
from jax.sharding import PartitionSpec as P

GROUPS = 4
LENGTH = 128


norm_eps = 1e-06


def norm_rows(values, gain):
    promoted = values.astype(jnp.float32)
    inverse = lax.rsqrt(jnp.mean(promoted * promoted, axis=-1, keepdims=True) + norm_eps)
    return (promoted * inverse * gain).astype(jnp.bfloat16)


def band_means(inputs, window, seq_length):
    row_count, columns = inputs.shape
    by_sequence = inputs.reshape(row_count // seq_length, seq_length, columns)
    position = jnp.arange(seq_length, dtype=jnp.int32)
    offset = position[:, None] - position[None, :]
    band_mask = ((offset >= 0) & (offset < window)).astype(jnp.bfloat16)
    divisor = jnp.minimum(position + 1, window).astype(jnp.float32)
    summed = jnp.einsum("ts,nsc->ntc", band_mask, by_sequence, preferred_element_type=jnp.float32)
    return (summed / divisor[None, :, None] - by_sequence.astype(jnp.float32)).reshape(
        row_count, columns
    )


def body(
    tokens,
    mix_gain,
    group_weight,
    group_scale,
    mlp_gain,
    up_weight,
    up_scale,
    down_weight,
    down_scale,
):
    model_width = tokens.shape[1]
    group_width = model_width // GROUPS
    own_cols = group_weight.shape[1]
    column_start = lax.axis_index("tp") * own_cols
    group_index = column_start // group_width
    normed = norm_rows(tokens, mix_gain)
    inputs = lax.dynamic_slice_in_dim(normed, group_index * group_width, group_width, 1)
    window = jnp.left_shift(jnp.int32(2), group_index)
    pooled = band_means(inputs, window, LENGTH).astype(jnp.bfloat16)
    mixed_cols = (
        jnp.dot(
            pooled,
            lax.all_gather(group_weight.astype(jnp.bfloat16), "fs", axis=0, tiled=True),
            preferred_element_type=jnp.float32,
        )
        * group_scale
    )
    own_tokens = lax.dynamic_slice_in_dim(tokens, column_start, own_cols, 1)
    carried_cols = (own_tokens.astype(jnp.float32) + mixed_cols).astype(jnp.bfloat16)
    carried = lax.all_gather(carried_cols, "tp", axis=1, tiled=True)
    normed_mlp = norm_rows(carried, mlp_gain)
    pre_act = (
        jnp.dot(
            normed_mlp,
            lax.all_gather(up_weight.astype(jnp.bfloat16), "fs", axis=0, tiled=True),
            preferred_element_type=jnp.float32,
        )
        * up_scale
    )
    hidden = jnp.square(jax.nn.relu(pre_act)).astype(jnp.bfloat16)
    partial_value = (
        jnp.dot(
            hidden,
            lax.all_gather(down_weight.astype(jnp.bfloat16), "fs", axis=1, tiled=True),
            preferred_element_type=jnp.float32,
        )
        * down_scale
    )
    summed = lax.psum(partial_value.astype(jnp.bfloat16), "tp").astype(jnp.float32)
    return (carried.astype(jnp.float32) + summed).astype(jnp.bfloat16)


MESH = pl.DeviceIdType.MESH


def ring_kernel(
    sizes,
    tok_h, mg, gw_h, gs, lg, up_h, us, dn_h, ds,
    out_h,
    tok, gwf, upf, upo, dnf, dno,
    gwg, ups, upg, dns, dng,
    car, xn, hid, pb, ra, sx, rb, sz, rc, og,
    ld, sw, rw, sy, ry, scz, rcz, scx, rcx, scc, rcc,
    sa, ra_s, sb, rb_s, st, rt, so, ro, wr,
):
    Z, T, rows, D, own, hg, hu, hd, fsub, dsub = sizes
    r, z, t = lax.axis_index("rep"), lax.axis_index("fs"), lax.axis_index("tp")
    cp = t + 1 - 2 * lax.rem(t, 2)
    xp = lax.rem(t + 2, T)
    cxp = lax.rem(cp + 2, T)
    peer_r = 1 - r
    bf, f32 = jnp.bfloat16, jnp.float32

    def mul(i, n):
        return pl.multiple_of(i * n, n)

    def zat(d):
        return lax.rem(z + d, Z)

    loads = {}

    def load(key, src, dst, k):
        c = pltpu.make_async_copy(src, dst, ld.at[k])
        c.start()
        loads[key] = c

    load("gw", gw_h, gwf, 0)
    load("tok", tok_h, tok, 1)
    order = list(range(1, Z)) + [0]
    for d in order:
        zd = zat(d)
        load(("up", d), up_h.at[pl.ds(mul(r, hu), hu), pl.ds(mul(zd, fsub), fsub)], upf.at[d], 2 + d)
    for d in order:
        zd = zat(d)
        load(("dn", d), dn_h.at[pl.ds(pl.multiple_of(zd * 2 * hd + r * hd, hd), hd), :], dnf.at[d], 2 + Z + d)
    load("upo", up_h.at[pl.ds(mul(peer_r, hu), hu), pl.ds(mul(z, fsub), fsub)], upo, 2 + 2 * Z)
    load("dno", dn_h.at[pl.ds(pl.multiple_of(z * 2 * hd + peer_r * hd, hd), hd), :], dno, 3 + 2 * Z)

    barrier = pltpu.get_barrier_semaphore()
    peers = [(r, zat(d), t) for d in range(1, Z)] + [(peer_r, z, t), (r, z, xp), (r, z, cp)]
    for p in peers:
        pl.semaphore_signal(barrier, inc=1, device_id=p, device_id_type=MESH)
    loads["gw"].wait()
    gwg[pl.ds(mul(z, 2 * hg), 2 * hg), :] = gwf[...].astype(bf)
    pl.semaphore_wait(barrier, len(peers))

    sends = []

    def remote(src, dst, ss, rs, dev):
        return pltpu.make_async_remote_copy(
            src_ref=src, dst_ref=dst, send_sem=ss, recv_sem=rs, device_id=dev, device_id_type=MESH
        )

    def send(src, dst, ss, rs, dev, when=None):
        if when is None:
            remote(src, dst, ss, rs, dev).start()
        else:
            pl.when(when)(lambda: remote(src, dst, ss, rs, dev).start())
        sends.append((when, (src, dst, ss, rs, dev)))

    def drain():
        for when, args in sends:
            if when is None:
                remote(*args).wait_send()
            else:
                pl.when(when)(lambda args=args: remote(*args).wait_send())

    def got(dst, ss, rs):
        remote(dst, dst, ss, rs, (peer_r, z, t)).wait_recv()

    def gw_at(src, rep):
        return gwg.at[pl.ds(pl.multiple_of(src * 2 * hg + rep * hg, hg), hg), :]

    def up_at(src, rep):
        return upg.at[pl.ds(pl.multiple_of(src * 2 * hu + rep * hu, hu), hu), :]

    def dn_at(src, rep):
        return dng.at[src, pl.ds(mul(rep, hd), hd), :]

    place = (gw_at, up_at, dn_at)

    for d in range(1, Z):
        send(gw_at(z, r), gw_at(z, r), sw.at[0, d], rw.at[0, z], (r, zat(d), t))
    ready = []
    for w, key, raw, cast in ((1, "up", upf, ups), (2, "dn", dnf, dns)):
        for d in range(1, Z):
            loads[(key, d)].wait()
            cast[d] = raw[d].astype(bf)
            ready.append((cast.at[d], place[w](z, r), sw.at[w, d], rw.at[w, z], (r, zat(d), t)))
            if w == 1 and d > 1 or w == 2 and d == 1:
                send(*ready.pop(0))
    loads[("up", 0)].wait()
    upg[pl.ds(pl.multiple_of(z * 2 * hu + r * hu, hu), hu), :] = upf[0].astype(bf)
    loads["upo"].wait()
    upg[pl.ds(pl.multiple_of(z * 2 * hu + peer_r * hu, hu), hu), :] = upo[...].astype(bf)
    loads[("dn", 0)].wait()
    dng[z, pl.ds(mul(r, hd), hd), :] = dnf[0].astype(bf)
    loads["dno"].wait()
    dng[z, pl.ds(mul(peer_r, hd), hd), :] = dno[...].astype(bf)

    loads["tok"].wait()
    full = tok[...].astype(f32)
    inv = lax.rsqrt(jnp.mean(full * full, axis=-1, keepdims=True) + norm_eps)
    cols = pl.ds(mul(t, own), own)
    mine = tok[:, cols].astype(f32)
    normed = (mine * inv * mg[:, cols]).astype(bf)
    window = jnp.left_shift(jnp.int32(2), t)
    ti = lax.broadcasted_iota(jnp.int32, (LENGTH, LENGTH), 0)
    si = lax.broadcasted_iota(jnp.int32, (LENGTH, LENGTH), 1)
    band = jnp.where((ti - si >= 0) & (ti - si < window), 1.0, 0.0).astype(bf)
    pos = lax.broadcasted_iota(jnp.int32, (LENGTH, own), 0)
    divisor = jnp.minimum(pos + 1, window).astype(f32)
    pooled = []
    for s in range(rows // LENGTH):
        part = normed[s * LENGTH:(s + 1) * LENGTH]
        summed = jnp.dot(band, part, preferred_element_type=f32)
        pooled.append((summed / divisor - part.astype(f32)).astype(bf))
    pooled = jnp.concatenate(pooled, axis=0)

    def swap_one(w, d):
        src = zat(Z - d)
        got(place[w](src, r), sw.at[w, d], rw.at[w, src])
        send(place[w](src, r), place[w](src, r), sy.at[w, d], ry.at[w, src], (peer_r, z, t))

    def swap(w):
        for d in range(1, Z):
            swap_one(w, d)

    def swapped(w):
        for d in range(1, Z):
            src = zat(Z - d)
            got(place[w](src, peer_r), sy.at[w, d], ry.at[w, src])

    swap(0)
    swapped(0)
    mixed = jnp.dot(pooled, gwg[...], preferred_element_type=f32) * gs[...]
    car[z, t] = (mine + mixed).astype(bf)
    H = rows // LENGTH
    hr = LENGTH
    side = 1 - 2 * lax.div(z, Z // 2)

    inner = lax.div(Z - 1 - side * (Z - 1 - 2 * z), 2)

    def src_of(d):
        if d == 0:
            return z
        near = (d + 1) // 2 if d % 2 else -(d // 2)
        both_sides = lax.div(2 * inner - d + 2 * Z, 2 * Z)
        return z + side * (both_sides * near + (1 - both_sides) * (d - inner))

    def half(h):
        return pl.ds(h * hr, hr)

    def to_x(src, h):
        b = car.at[src, t, half(h)]
        send(b, b, scx.at[src, h], rcx.at[src, h], (r, z, xp))

    def to_core(src, h, q, k):
        b = car.at[src, q, half(h)]
        send(b, b, scc.at[src, k, h], rcc.at[src, k, h], (r, z, cp))

    def to_z(src, h, when_up, when_down):
        b = car.at[src, t, half(h)]
        send(b, b, scz.at[0, src, h], rcz.at[src, h], (r, lax.rem(z + 1, Z), t), when_up)
        send(b, b, scz.at[1, src, h], rcz.at[src, h], (r, lax.rem(z + Z - 1, Z), t), when_down)

    for h in range(H):
        to_z(z, h, z < Z - 1, z > 0)
        to_x(z, h)
        to_core(z, h, t, 0)
    for args in ready:
        send(*args)

    def arrive(d, h):
        src = src_of(d)
        got(car.at[src, t, half(h)], scz.at[0, src, h], rcz.at[src, h])
        to_z(src, h, (src < z) & (z < Z - 1), (src > z) & (z > 0))
        to_x(src, h)
        to_core(src, h, t, 0)

    def from_x(d, h):
        src = src_of(d)
        got(car.at[src, xp, half(h)], scx.at[src, h], rcx.at[src, h])
        to_core(src, h, xp, 1)

    swap(1)
    for h in range(H):
        from_x(0, h)
    for d in range(1, Z):
        for h in range(H):
            arrive(d, h)
            if d > 1:
                from_x(d - 1, h)
        swap_one(2, d)
    for h in range(H):
        from_x(Z - 1, h)
    swapped(1)

    def up(d, h):
        src = src_of(d)
        hs = half(h)
        got(car.at[src, cp, hs], scc.at[src, 0, h], rcc.at[src, 0, h])
        got(car.at[src, cxp, hs], scc.at[src, 1, h], rcc.at[src, 1, h])
        total = jnp.zeros((hr, 1), f32)
        for q in range(T):
            c = car[src, q, hs].astype(f32)
            total += jnp.sum(c * c, axis=-1, keepdims=True)
        scale = lax.rsqrt(total / D + norm_eps)
        for q in range(T):
            part = slice(q * own, (q + 1) * own)
            xn[:, part] = (car[src, q, hs].astype(f32) * scale * lg[:, part]).astype(bf)
        pre = jnp.dot(xn[...], upg[...], preferred_element_type=f32)
        pre = jnp.maximum(pre * us[:, pl.ds(mul(z, fsub), fsub)], 0.0)
        hid[src, hs] = (pre * pre).astype(bf)

    def down(d, h):
        src = src_of(d)
        hs = half(h)
        hidden = hid[src, hs]
        for q in range(T):
            part = slice(q * own, (q + 1) * own)
            p = jnp.dot(hidden, dng[q], preferred_element_type=f32) * ds[:, part]
            pb[src, q, hs] = p.astype(bf)
        for k, q in ((1, cxp), (0, cp)):
            send(pb.at[src, q, hs], ra.at[src, k, hs], sa.at[src, k, h], ra_s.at[src, k, h], (r, z, cp))

    def over_x(d, h):
        src = src_of(d)
        hs = half(h)
        got(ra.at[src, 1, hs], sa.at[src, 1, h], ra_s.at[src, 1, h])
        sx[src, hs] = (pb[src, xp, hs].astype(f32) + ra[src, 1, hs].astype(f32)).astype(bf)
        send(sx.at[src, hs], rb.at[src, hs], sb.at[src, h], rb_s.at[src, h], (r, z, xp))

    def over_z(d, h):
        src = src_of(d)
        hs = half(h)
        got(ra.at[src, 0, hs], sa.at[src, 0, h], ra_s.at[src, 0, h])
        got(rb.at[src, hs], sb.at[src, h], rb_s.at[src, h])
        both = pb[src, t, hs].astype(f32) + ra[src, 0, hs].astype(f32) + rb[src, hs].astype(f32)
        if d == 0:
            return both
        sz[src, hs] = both.astype(bf)
        send(sz.at[src, hs], rc.at[z, hs], st.at[src, h], rt.at[z, h], (r, src, t))

    for d in range(Z):
        for h in range(H):
            up(d, h)
    swapped(2)
    units = [(d, h) for d in range(Z - 1, -1, -1) for h in range(H)]
    stages = (down, over_x, over_z)
    for i in range(len(units) + len(stages) - 1):
        for lag, stage in enumerate(stages):
            if 0 <= i - lag < len(units):
                d, h = units[i - lag]
                if d > 0 or stage is not over_z:
                    stage(d, h)

    writes = []

    def write(q, k, h):
        c = pltpu.make_async_copy(
            og.at[q, half(h)], out_h.at[half(h), pl.ds(mul(q, own), own)], wr.at[k, h]
        )
        c.start()
        writes.append(c)

    def pass_on(q, k, dev, h):
        b = og.at[q, half(h)]
        send(b, b, so.at[k, h], ro.at[k, h], dev)

    for h in range(H):
        hs = half(h)
        acc = over_z(0, h) + car[z, t, hs].astype(f32)
        for d in range(1, Z):
            src = src_of(d)
            got(rc.at[src, hs], st.at[src, h], rt.at[src, h])
            acc += rc[src, hs].astype(f32)
        og[t, hs] = acc.astype(bf)
        pass_on(t, 0, (r, z, xp), h)
        pass_on(t, 1, (r, z, cp), h)
        write(t, 0, h)
    for h in range(H):
        got(og.at[xp, half(h)], so.at[0, h], ro.at[0, h])
        pass_on(xp, 2, (r, z, cp), h)
        write(xp, 1, h)
    for h in range(H):
        got(og.at[cp, half(h)], so.at[1, h], ro.at[1, h])
        write(cp, 2, h)
        got(og.at[cxp, half(h)], so.at[2, h], ro.at[2, h])
        write(cxp, 3, h)
    drain()
    for c in writes:
        c.wait()


def fused(mesh_shape, tokens, mix_gain, group_weight, group_scale, mlp_gain, up_weight, up_scale, down_weight, down_scale):
    Z, T = mesh_shape["fs"], mesh_shape["tp"]
    rows, D = tokens.shape
    own = group_weight.shape[1]
    hg, hu = group_weight.shape[0] // 2, up_weight.shape[0] // 2
    fsub = up_weight.shape[1] // Z
    hd = fsub // 2
    dsub = down_weight.shape[1]
    bf, f32 = jnp.bfloat16, jnp.float32
    dma = pltpu.SemaphoreType.DMA
    vm = pl.BlockSpec(memory_space=pltpu.VMEM)
    hbm = pl.BlockSpec(memory_space=pl.ANY)
    sizes = (Z, T, rows, D, own, hg, hu, hd, fsub, dsub)
    V = pltpu.VMEM
    block = (Z, rows, own)
    H = rows // LENGTH
    return pl.pallas_call(
        functools.partial(ring_kernel, sizes),
        out_shape=jax.ShapeDtypeStruct((rows, D), bf),
        in_specs=[hbm, vm, hbm, vm, vm, hbm, vm, hbm, vm],
        out_specs=hbm,
        scratch_shapes=[
            V((rows, D), bf), V((2 * hg, own), f32),
            V((Z, hu, fsub), f32), V((hu, fsub), f32), V((Z, hd, dsub), f32), V((hd, dsub), f32),
            V((Z * 2 * hg, own), bf), V((Z, hu, fsub), bf), V((Z * 2 * hu, fsub), bf),
            V((Z, hd, dsub), bf), V((Z, 2 * hd, dsub), bf),
            V((Z, T, rows, own), bf), V((LENGTH, D), bf), V((Z, rows, fsub), bf), V((Z, T, rows, own), bf),
            V((Z, 2, rows, own), bf), V(block, bf), V(block, bf), V(block, bf), V(block, bf),
            V((T, rows, own), bf),
            dma((4 + 2 * Z,)), dma((3, Z)), dma((3, Z)), dma((3, Z)), dma((3, Z)),
            dma((2, Z, H)), dma((Z, H)), dma((Z, H)), dma((Z, H)), dma((Z, 2, H)), dma((Z, 2, H)),
            dma((Z, 2, H)), dma((Z, 2, H)), dma((Z, H)), dma((Z, H)), dma((Z, H)), dma((Z, H)),
            dma((3, H)), dma((3, H)), dma((4, H)),
        ],
        compiler_params=pltpu.CompilerParams(
            collective_id=0, has_side_effects=True, vmem_limit_bytes=60 * 1024 * 1024
        ),
    )(
        tokens, mix_gain[None], group_weight, group_scale, mlp_gain[None],
        up_weight, up_scale, down_weight, down_scale,
    )


def fits(mesh):
    shape = mesh.shape
    return shape["rep"] == 2 and shape["tp"] == GROUPS and shape["fs"] == shape["tp"]


def solution(mesh):
    in_specs = (
        P(("rep", "fs"), None),
        P(),
        P("fs", "tp"),
        P(None, "tp"),
        P(),
        P("fs", "tp"),
        P(None, "tp"),
        P("tp", "fs"),
        P(),
    )
    out_specs = P(("rep", "fs"), None)
    chosen = functools.partial(fused, mesh.shape) if fits(mesh) else body
    return jax.shard_map(chosen, mesh=mesh, in_specs=in_specs, out_specs=out_specs, check_vma=False)
```
